32 devices in a mesh: rep: 2 (over x), fs: 8 (over z, y), tp: 2 (over core).
Axes of the slice: x: 2, y: 2, z: 4, core: 2. Of those that a mesh axis runs over, the one named last changes fastest.
Arguments:
- later_input: bfloat16 [8192, 2048], P(('rep', 'fs', 'tp')), may hold values from -6 to 6
- earlier_input: bfloat16 [8192, 2048], P(('rep', 'fs', 'tp')), may hold values from -6 to 6
- hidden_cot: bfloat16 [8192, 2816], P(('rep', 'fs'), 'tp'), may hold values from -8 to 8
- norm_gain: float32 [2048], replicated, may hold values from 0.1 to 1.9
- gate_weight: bfloat16 [2048, 2816], P('fs', 'tp'), may hold values from -0.125 to 0.125
- up_weight: bfloat16 [2048, 2816], P('fs', 'tp'), may hold values from -0.125 to 0.125
- gate_running: float32 [2048, 2816], P('fs', 'tp'), may hold values from -6 to 6
- up_running: float32 [2048, 2816], P('fs', 'tp'), may hold values from -6 to 6
- gain_running: float32 [2048], replicated, may hold values from -6 to 6
Outputs:
- later_hidden: bfloat16 [8192, 2816], P(('rep', 'fs'), 'tp')
- earlier_grad: bfloat16 [8192, 2048], P(('rep', 'fs', 'tp'))
- gate_total: float32 [2048, 2816], P('fs', 'tp')
- up_total: float32 [2048, 2816], P('fs', 'tp')
- gain_total: float32 [2048], replicated
The draws below stay inside these ranges and needn't reach their ends.
All inputs are finite; a program needn't handle non-finite values.
Results may differ from the reference program's by a relative error of at most 0.015.
Values may be sent and summed in bfloat16 or wider, within the bound.
No kernel may reach another device: no remote copies, remote signals or barrier semaphores. Data moves between devices by JAX's collectives and lax.ppermute only.
A program may use at most 128 MiB of HBM per device.

```python
import math
import jax
import jax.numpy as jnp
from jax import lax

D = 2048
HIDDEN_SIZE = 2816
HIDDEN_TP = 1408
TOKENS = 8192
N_TP = 2


def raised(array, stream_key, source, target, shards_of, factor):
    owner, partner = [(jnp.arange(array.shape[dim]) // (array.shape[dim] // shards_of)).reshape([-1 if axis == dim else 1 for axis in range(array.ndim)]) for dim in (source, target)]
    chosen = jax.random.permutation(stream_key, shards_of)[partner]
    strong = (owner == chosen) | (owner == (partner + shards_of // 2) % shards_of)
    return jnp.where(strong, factor * array, array)


def shard_levels(rng, shape, cuts, smallest, largest):
    def one(axis_at, blocks):
        steps = jax.random.uniform(jax.random.fold_in(jax.random.fold_in(rng, 6), axis_at), (blocks,), jnp.float32, smallest / len(cuts), largest / len(cuts))
        return jnp.repeat(jnp.exp(steps), shape[axis_at] // blocks).reshape((-1,) + (1,) * (len(shape) - axis_at - 1))

    gain = one(*cuts[0])
    for cut in cuts[1:]:
        gain = gain * one(*cut)
    return gain


def normal_values(key, dims, spread, reach, split=(), kind=jnp.bfloat16):
    array = jax.random.normal(key, dims, jnp.float32) * spread
    if len(split) > 0:
        array = shard_levels(key, dims, split, -0.22, 0.18) * array
    return jnp.clip(array, min=-reach, max=reach).astype(kind)


def bell_draw_with(rng, dims, scale, bound, shards, heavy, dtype=jnp.bfloat16):
    values = scale * jax.random.normal(rng, dims, jnp.float32)
    if shards:
        values = values * shard_levels(rng, dims, shards, -0.22, 0.18)
    return jnp.clip(raised(values, jax.random.fold_in(rng, 3), *heavy), -bound, bound).astype(dtype)


def setup_inputs(seed: int = 0) -> dict:
    seeds = jax.random.split(jax.random.key(seed), 10)
    return {
        "later_input": normal_values(seeds[0], (TOKENS, D), 1.0, 6.0, ((0, 32),)),
        "earlier_input": normal_values(seeds[1], (TOKENS, D), 1.0, 6.0, ((0, 32),)),
        "hidden_cot": bell_draw_with(seeds[2], (TOKENS, HIDDEN_SIZE), 1.0, 8.0, ((0, 16), (1, 2)), (0, 1, 16, 2.0)),
        "norm_gain": jnp.clip(1.0 + 0.18 * jax.random.normal(seeds[3], (D,), jnp.float32), 0.1, 1.9),
        "gate_weight": normal_values(seeds[4], (D, HIDDEN_SIZE), D ** -0.5, 0.125, ((0, 8), (1, 2))),
        "up_weight": normal_values(seeds[5], (D, HIDDEN_SIZE), D ** -0.5, 0.125, ((0, 8), (1, 2))),
        "gate_running": normal_values(seeds[6], (D, HIDDEN_SIZE), 1.0, 6.0, ((0, 8), (1, 2)), jnp.float32),
        "up_running": normal_values(seeds[7], (D, HIDDEN_SIZE), 1.0, 6.0, ((0, 8), (1, 2)), jnp.float32),
        "gain_running": normal_values(seeds[8], (D,), 1.0, 6.0, (), jnp.float32),
    }


EPSILON = 1e-06

def normalize(activation, norm_gain):
    values = activation.astype(jnp.float32)
    inv_rms = lax.rsqrt(lax.optimization_barrier(jnp.mean(values * values, axis=1, keepdims=True)) + EPSILON)
    return (values, inv_rms, (values * inv_rms * norm_gain).astype(jnp.bfloat16))

def reference(later_input, earlier_input, hidden_cot, norm_gain, gate_weight, up_weight, gate_running, up_running, gain_running):
    factor = 1.0 / math.sqrt(TOKENS)
    later_vals, later_inv, later_norm = normalize(later_input, norm_gain)
    later_gate = jnp.dot(later_norm, gate_weight, preferred_element_type=jnp.float32)
    later_up = jnp.dot(later_norm, up_weight, preferred_element_type=jnp.float32)
    later_hidden = (jax.nn.silu(later_gate) * later_up).astype(jnp.bfloat16)
    earlier_vals, earlier_inv, earlier_norm = normalize(earlier_input, norm_gain)
    earlier_gate = jnp.dot(earlier_norm, gate_weight, preferred_element_type=jnp.float32)
    earlier_up = jnp.dot(earlier_norm, up_weight, preferred_element_type=jnp.float32)
    gate_sigmoid = jax.nn.sigmoid(earlier_gate)
    upstream = hidden_cot.astype(jnp.float32)
    d_up = (upstream * earlier_gate * gate_sigmoid).astype(jnp.bfloat16)
    d_gate = (upstream * earlier_up * gate_sigmoid * (1.0 + earlier_gate * (1.0 - gate_sigmoid))).astype(jnp.bfloat16)
    d_norm = jnp.zeros((TOKENS, D), jnp.float32)
    for column_block in range(N_TP):
        first_col = column_block * HIDDEN_TP
        partial_sum = jnp.dot(d_gate[:, first_col:first_col + HIDDEN_TP], gate_weight[:, first_col:first_col + HIDDEN_TP].T, preferred_element_type=jnp.float32)
        partial_sum = partial_sum + jnp.dot(d_up[:, first_col:first_col + HIDDEN_TP], up_weight[:, first_col:first_col + HIDDEN_TP].T, preferred_element_type=jnp.float32)
        rounded = lax.optimization_barrier(partial_sum.astype(jnp.bfloat16))
        d_norm = d_norm + rounded.astype(jnp.float32)
    scaled = d_norm * norm_gain
    inner = lax.optimization_barrier(jnp.mean(scaled * earlier_vals, axis=1, keepdims=True))
    earlier_grad = (earlier_inv * scaled - earlier_vals * earlier_inv ** 3 * inner).astype(jnp.bfloat16)
    gate_total = gate_running + factor * jnp.dot(earlier_norm.T, d_gate, preferred_element_type=jnp.float32)
    up_total = up_running + factor * jnp.dot(earlier_norm.T, d_up, preferred_element_type=jnp.float32)
    gain_total = gain_running + factor * lax.optimization_barrier(jnp.sum(d_norm * earlier_vals * earlier_inv, axis=0))
    return (later_hidden, earlier_grad, gate_total, up_total, gain_total)
```

```python
import functools
import math

import jax
import jax.numpy as jnp
from jax import lax
from jax.experimental import pallas as pl
from jax.experimental.pallas import tpu as pltpu
from jax.sharding import PartitionSpec as P

EPSILON = 1e-06
LANES = 128
VMEM = pl.BlockSpec(memory_space=pltpu.VMEM)
SMEM = pl.BlockSpec(memory_space=pltpu.SMEM)
F32 = jnp.float32
BF16 = jnp.bfloat16
CONTRACT_ROWS = (((0,), (0,)), ((), ()))
CONTRACT_COLS = (((1,), (1,)), ((), ()))


def call(kernel, out_shape, in_specs, args, name, flops=0, moved=0, out_specs=None, grid=None, scratch=()):
    extra = {} if grid is None else {"grid": grid}
    if out_specs is None:
        out_specs = jax.tree.map(lambda _: VMEM, out_shape)
    return pl.pallas_call(
        kernel,
        out_shape=out_shape,
        in_specs=in_specs,
        out_specs=out_specs,
        scratch_shapes=scratch,
        name=name,
        cost_estimate=pl.CostEstimate(flops=flops, bytes_accessed=moved, transcendentals=0),
        **extra,
    )(*args)


def low_half(shape):
    return lax.broadcasted_iota(jnp.int32, shape, 1) % LANES < LANES // 2


def swap_halves(block):
    return pltpu.roll(block, LANES // 2, 1)


def inverse_rms(values):
    return lax.rsqrt(jnp.mean(values * values, axis=1, keepdims=True) + EPSILON)


def pack_weights_kernel(main, place, gate_ref, up_ref, out_ref):
    member = place[0]
    start = pl.multiple_of(member * main, LANES)
    out_ref[:, :main] = gate_ref[:, pl.ds(start, main)]
    out_ref[:, main : 2 * main] = up_ref[:, pl.ds(start, main)]
    gate = gate_ref[:, 2 * main :].astype(F32)
    up = up_ref[:, 2 * main :].astype(F32)
    low = low_half(gate.shape)
    first = jnp.where(low, gate, swap_halves(up))
    second = jnp.where(low, swap_halves(gate), up)
    out_ref[:, 2 * main :] = jnp.where(member == 0, first, second).astype(BF16)


def pack_cot_kernel(main, place, cot_ref, mine_ref, theirs_ref):
    member, core = place[0], place[1]
    rows = cot_ref.shape[0] // 2
    for half in range(2):
        source = pl.ds(pl.multiple_of((core if half == 0 else 1 - core) * rows, rows), rows)
        target = pl.ds(half * rows, rows)
        tail = cot_ref[source, 2 * main :].astype(F32)
        turned = swap_halves(tail)
        low = low_half(tail.shape)
        tails = (jnp.where(low, tail, turned), jnp.where(low, turned, tail))
        for ref, who in ((mine_ref, member), (theirs_ref, 1 - member)):
            ref[target, :main] = cot_ref[source, pl.ds(pl.multiple_of(who * main, LANES), main)]
            ref[target, main:] = jnp.where(who == 0, tails[0], tails[1]).astype(BF16)


def norm_kernel(blocks, order, gain_ref, *refs):
    out_ref = refs[-1]
    rows, width = refs[0].shape
    cut = width // blocks
    for at, ref in enumerate(refs[:-1]):
        values = ref[...].astype(F32)
        inv = inverse_rms(values)
        for slot in range(blocks):
            source = pl.ds(pl.multiple_of(order[slot] * cut, LANES), cut)
            out_ref[at * rows : (at + 1) * rows, slot * cut : (slot + 1) * cut] = (
                ref[:, source].astype(F32) * inv * gain_ref[:, source]
            ).astype(BF16)


def back_pointwise(gate, up, cot):
    sig = 1.0 / (1.0 + jnp.exp(-gate))
    both = cot * sig
    return both * up * (1.0 + gate * (1.0 - sig)), both * gate


def back_kernel(main, count, acc_ref, norm_ref, *refs):
    weights, cot_ref, out_ref = refs[:count], refs[count], refs[count + 1]
    cut = weights[0].shape[0]
    total = acc_ref[...]
    for at, ref in enumerate(weights):
        total = total + jnp.dot(norm_ref[:, at * cut : (at + 1) * cut], ref[...], preferred_element_type=F32)
    cot = cot_ref[...].astype(F32)
    d_gate, d_up = back_pointwise(total[:, :main], total[:, main : 2 * main], cot[:, :main])
    out_ref[:, :main] = d_gate.astype(BF16)
    out_ref[:, main : 2 * main] = d_up.astype(BF16)
    tail = total[:, 2 * main :]
    turned = swap_halves(tail)
    low = low_half(tail.shape)
    d_gate, d_up = back_pointwise(jnp.where(low, tail, turned), jnp.where(low, turned, tail), cot[:, main:])
    out_ref[:, 2 * main :] = jnp.where(low, d_gate, d_up).astype(BF16)


def forward_kernel(main, norm_ref, weight_ref, out_ref):
    total = jnp.dot(norm_ref[...], weight_ref[...], preferred_element_type=F32)
    gate, up = total[:, :main], total[:, main : 2 * main]
    out_ref[:, :main] = (gate / (1.0 + jnp.exp(-gate)) * up).astype(BF16)
    tail = total[:, 2 * main :]
    turned = swap_halves(tail)
    low = low_half(tail.shape)
    gate, up = jnp.where(low, tail, turned), jnp.where(low, turned, tail)
    out_ref[:, main:] = (gate / (1.0 + jnp.exp(-gate)) * up).astype(BF16)


def hidden_kernel(main, place, mine_ref, theirs_ref, out_ref):
    member, core = place[0], place[1]
    rows = mine_ref.shape[0] // 2
    for half in range(2):
        target = pl.ds(pl.multiple_of((core if half == 0 else 1 - core) * rows, rows), rows)
        source = pl.ds(half * rows, rows)
        out_ref[target, pl.ds(pl.multiple_of(member * main, LANES), main)] = mine_ref[source, :main]
        out_ref[target, pl.ds(pl.multiple_of((1 - member) * main, LANES), main)] = theirs_ref[source, :main]
        mine, theirs = mine_ref[source, main:], theirs_ref[source, main:]
        keep = low_half(mine.shape) == (member == 0)
        out_ref[target, 2 * main :] = jnp.where(keep, mine.astype(F32), theirs.astype(F32)).astype(BF16)


def input_grad_kernel(blocks, order, raw_ref, own_ref, other_ref, gain_ref, out_ref, sum_ref):
    width = raw_ref.shape[1]
    cut = width // blocks
    values = raw_ref[...].astype(F32)
    inv = inverse_rms(values)
    inner = jnp.zeros_like(inv)
    for slot in range(blocks):
        source = pl.ds(pl.multiple_of(order[slot] * cut, LANES), cut)
        held = slice(slot * cut, (slot + 1) * cut)
        d_norm = own_ref[:, held].astype(F32) + other_ref[:, held].astype(F32)
        raw = raw_ref[:, source].astype(F32)
        sum_ref[:, source] = jnp.sum(d_norm * raw * inv, axis=0, keepdims=True)
        inner = inner + jnp.sum(d_norm * gain_ref[:, source] * raw, axis=1, keepdims=True)
    inner = inner / width * (inv * inv * inv)
    for slot in range(blocks):
        source = pl.ds(pl.multiple_of(order[slot] * cut, LANES), cut)
        held = slice(slot * cut, (slot + 1) * cut)
        d_norm = own_ref[:, held].astype(F32) + other_ref[:, held].astype(F32)
        out_ref[:, source] = (
            inv * (d_norm * gain_ref[:, source]) - raw_ref[:, source].astype(F32) * inner
        ).astype(BF16)


def total_kernel(main, factor, place, mine_ref, theirs_ref, gate_ref, up_ref, gate_out, up_out):
    member = place[0]
    for ref, who in ((mine_ref, member), (theirs_ref, 1 - member)):
        target = pl.ds(pl.multiple_of(who * main, LANES), main)
        gate_out[:, target] = gate_ref[:, target] + factor * ref[:, :main].astype(F32)
        up_out[:, target] = up_ref[:, target] + factor * ref[:, main : 2 * main].astype(F32)
    mine, theirs = mine_ref[:, 2 * main :].astype(F32), theirs_ref[:, 2 * main :].astype(F32)
    first, second = jnp.where(member == 0, mine, theirs), jnp.where(member == 0, theirs, mine)
    low = low_half(first.shape)
    tail = slice(2 * main, None)
    gate_out[:, tail] = gate_ref[:, tail] + factor * jnp.where(low, first, swap_halves(second))
    up_out[:, tail] = up_ref[:, tail] + factor * jnp.where(low, swap_halves(first), second)


def body(
    later_input,
    earlier_input,
    hidden_cot,
    norm_gain,
    gate_weight,
    up_weight,
    gate_running,
    up_running,
    gain_running,
):
    local_rows, width = later_input.shape
    shard, width_tp = gate_weight.shape
    count_rep = lax.axis_size("rep")
    count_fs = lax.axis_size("fs")
    count_tp = lax.axis_size("tp")
    factor = 1.0 / math.sqrt(local_rows * count_rep * count_fs * count_tp)
    assert count_rep == 2 and count_tp == 2 and width_tp % (2 * LANES) == LANES
    main = width_tp // (2 * LANES) * LANES
    padded = main + LANES
    pair_rows = 2 * local_rows
    all_rows = 4 * local_rows
    member, place_fs, core = lax.axis_index("rep"), lax.axis_index("fs"), lax.axis_index("tp")
    place = jnp.stack([member, core]).astype(jnp.int32)
    gain_row = norm_gain.reshape(1, width)

    swap = [(0, 1), (1, 0)]
    over_rep = lambda value: lax.ppermute(value, "rep", swap)
    over_tp = lambda value: lax.ppermute(value, "tp", swap)
    columns = 2
    line = count_fs // columns
    lined = line == 4 and shard % LANES == 0

    def fs_pairs(moves):
        return [(a * columns + b, c * columns + b) for a, c in moves for b in range(columns)]

    near = fs_pairs([(0, 1), (1, 0), (2, 3), (3, 2)])
    middle = fs_pairs([(1, 2), (2, 1)])
    outward = fs_pairs([(1, 0), (2, 3)])
    inward = fs_pairs([(0, 1), (3, 2)])
    across = [(a * columns + b, a * columns + 1 - b) for a in range(line) for b in range(columns)]
    far = fs_pairs([(0, 2), (2, 0), (1, 3), (3, 1)])
    over_fs = lambda value, pairs: lax.ppermute(value, "fs", pairs)

    packed = call(
        functools.partial(pack_weights_kernel, main),
        jax.ShapeDtypeStruct((shard, width_tp), BF16),
        [SMEM, VMEM, VMEM],
        (place, gate_weight, up_weight),
        "pack_weights",
        moved=6 * shard * width_tp,
    )
    if lined:
        row, column = place_fs // columns, place_fs % columns
        upper = row >= line // 2
        edge = (row == 0) | (row == line - 1)
        rows_of = [
            row,
            row + 1 - 2 * (row % 2),
            jnp.where(upper, 1, 2),
            jnp.where(upper, 0, 3),
        ]
        order = jnp.stack(
            [at * columns + (column if side == 0 else 1 - column) for at in rows_of for side in range(2)]
        ).astype(jnp.int32)
        by_near = over_fs(packed, near)
        by_middle = over_fs(packed, middle)
        by_middle_far = over_fs(by_near, middle)
        third = jnp.where(edge, over_fs(by_middle, outward), by_middle)
        fourth = jnp.where(edge, over_fs(by_middle_far, outward), by_middle_far)
        slots = []
        for block in (packed, by_near, third, fourth):
            slots += [block, over_fs(block, across)]
        cut = shard
    else:
        order = jnp.arange(count_fs, dtype=jnp.int32)
        whole = lax.all_gather(packed, "fs", axis=0, tiled=True)
        slots = [whole]
        cut = width
        order = jnp.zeros((1,), jnp.int32)
    blocks = len(slots)

    def rows_of_group(own):
        beyond = over_rep(own)
        return (own, over_tp(own), beyond, over_tp(beyond))

    def normalized(own, name):
        return call(
            functools.partial(norm_kernel, blocks),
            jax.ShapeDtypeStruct((all_rows, width), BF16),
            [SMEM] + [VMEM] * 5,
            (order, gain_row) + rows_of_group(own),
            name,
            moved=4 * all_rows * width,
            flops=20 * all_rows * width,
        )

    earlier_norm = normalized(earlier_input, "norm_earlier")
    cot_mine, cot_theirs = call(
        functools.partial(pack_cot_kernel, main),
        (jax.ShapeDtypeStruct((pair_rows, padded), BF16),) * 2,
        [SMEM, VMEM],
        (place, hidden_cot),
        "pack_cot",
        moved=4 * pair_rows * width_tp,
    )
    cot = jnp.concatenate([cot_mine, over_rep(cot_theirs)], axis=0)
    later_norm = normalized(later_input, "norm_later")

    tail_count = 2 if lined else 1
    early = blocks - tail_count
    acc = jnp.zeros((all_rows, width_tp), F32)
    for at in range(early):
        acc = acc + jnp.dot(earlier_norm[:, at * cut : (at + 1) * cut], slots[at], preferred_element_type=F32)
    tile = local_rows
    tail_width = tail_count * cut
    tail_at = early // tail_count
    whole_block = lambda shape: pl.BlockSpec(shape, lambda i: (0, 0))
    d_both = call(
        functools.partial(back_kernel, main, tail_count),
        jax.ShapeDtypeStruct((all_rows, width_tp), BF16),
        [pl.BlockSpec((tile, width_tp), lambda i: (i, 0)), pl.BlockSpec((tile, tail_width), lambda i: (i, tail_at))]
        + [whole_block((cut, width_tp))] * tail_count
        + [pl.BlockSpec((tile, padded), lambda i: (i, 0))],
        (acc, earlier_norm, *slots[early:], cot),
        "back",
        flops=2 * all_rows * tail_width * width_tp,
        moved=8 * all_rows * width_tp,
        out_specs=pl.BlockSpec((tile, width_tp), lambda i: (i, 0)),
        grid=(all_rows // tile,),
    )

    def term(at):
        return lax.dot_general(
            earlier_norm[:, at * cut : (at + 1) * cut], d_both, CONTRACT_ROWS, preferred_element_type=F32
        ).astype(BF16)

    def plus(*values):
        return sum(value.astype(F32) for value in values)

    if lined:
        halves = {}
        for at in (3, 2, 1, 0):
            sent = over_fs(term(2 * at + 1), across)
            halves[at] = plus(term(2 * at), sent)
        narrow = {at: value.astype(BF16) for at, value in halves.items()}
        third_in, fourth_in = over_fs(narrow[2], inward), over_fs(narrow[3], inward)
        fourth_sum = plus(narrow[3], fourth_in).astype(BF16)
        third_sum = plus(narrow[2], third_in).astype(BF16)
        fourth_got = over_fs(fourth_sum, middle)
        third_got = over_fs(third_sum, middle)
        second_sum = plus(narrow[1], fourth_got).astype(BF16)
        own_sum = plus(narrow[0], third_got, over_fs(second_sum, near)).astype(BF16)
    else:
        own_sum = lax.psum_scatter(term(0), "fs", scatter_dimension=0, tiled=True)
    gate_total, up_total = call(
        functools.partial(total_kernel, main, factor),
        (jax.ShapeDtypeStruct((shard, width_tp), F32),) * 2,
        [SMEM] + [VMEM] * 4,
        (place, own_sum, over_rep(own_sum), gate_running, up_running),
        "totals",
        moved=20 * shard * width_tp,
    )

    whole = slots[0] if blocks == 1 else jnp.concatenate(slots, axis=0)
    d_rows = lax.dot_general(d_both, whole, CONTRACT_COLS, preferred_element_type=F32).astype(BF16)
    d_rows = d_rows.reshape(2, 2, local_rows, width)
    summed = plus(d_rows[:, 0], over_tp(d_rows[:, 1])).astype(BF16)
    earlier_grad, gain_local = call(
        functools.partial(input_grad_kernel, blocks),
        (jax.ShapeDtypeStruct((local_rows, width), BF16), jax.ShapeDtypeStruct((1, width), F32)),
        [SMEM] + [VMEM] * 4,
        (order, earlier_input, summed[0], over_rep(summed[1]), gain_row),
        "input_grad",
        moved=8 * local_rows * width,
    )
    if lined:
        gain_sum = gain_local
        gain_sum = gain_sum + over_tp(gain_sum)
        gain_sum = gain_sum + over_rep(gain_sum)
        for pairs in (across, near, far):
            gain_sum = gain_sum + over_fs(gain_sum, pairs)
    else:
        gain_sum = lax.psum(gain_local, ("rep", "fs", "tp"))
    gain_total = gain_running + factor * gain_sum.reshape(width)

    hidden = call(
        functools.partial(forward_kernel, main),
        jax.ShapeDtypeStruct((all_rows, padded), BF16),
        [pl.BlockSpec((tile, width), lambda i: (i, 0)), whole_block((width, width_tp))],
        (later_norm, whole),
        "forward",
        flops=2 * all_rows * width * width_tp,
        moved=4 * all_rows * width,
        out_specs=pl.BlockSpec((tile, padded), lambda i: (i, 0)),
        grid=(all_rows // tile,),
    )
    later_hidden = call(
        functools.partial(hidden_kernel, main),
        jax.ShapeDtypeStruct((pair_rows, width_tp), BF16),
        [SMEM, VMEM, VMEM],
        (place, hidden[:pair_rows], over_rep(hidden[pair_rows:])),
        "hidden_out",
        moved=4 * pair_rows * width_tp,
    )
    return (later_hidden, earlier_grad, gate_total, up_total, gain_total)


def solution(mesh):
    in_specs = (
        P(("rep", "fs", "tp"), None),
        P(("rep", "fs", "tp"), None),
        P(("rep", "fs"), "tp"),
        P(),
        P("fs", "tp"),
        P("fs", "tp"),
        P("fs", "tp"),
        P("fs", "tp"),
        P(),
    )
    out_specs = (
        P(("rep", "fs"), "tp"),
        P(("rep", "fs", "tp"), None),
        P("fs", "tp"),
        P("fs", "tp"),
        P(),
    )
    return jax.shard_map(body, mesh=mesh, in_specs=in_specs, out_specs=out_specs, check_vma=False)
```
